32 devices in a mesh: fs: 8 (over z, x), tp: 4 (over y, core).
Axes of the slice: x: 2, y: 2, z: 4, core: 2. Of those that a mesh axis runs over, the one named last changes fastest.
Arguments:
- tokens: bfloat16 [1024, 2048], P('fs'), may hold values from -6 to 6
- route_ids: int32 [1024, 2], P('fs'), may hold values from 0 to 15, as said below
- route_weights: float32 [1024, 2], P('fs'), may hold values from 0.05 to 0.6
- norm_gain: float32 [2048], P('fs'), may hold values from 0.1 to 1.9
- gate_weight: float32 [16, 2048, 1024], P(None, 'fs', 'tp'), may hold values from -6 to 6
- up_weight: float32 [16, 2048, 1024], P(None, 'fs', 'tp'), may hold values from -6 to 6
- down_weight: float32 [16, 2048, 1024], P(None, 'fs', 'tp'), may hold values from -6 to 6
Outputs:
- gate_served: bfloat16 [16, 2048, 1024], P('fs', None, 'tp')
- up_served: bfloat16 [16, 2048, 1024], P('fs', None, 'tp')
- down_served: bfloat16 [16, 2048, 1024], P('fs', None, 'tp')
- combined: bfloat16 [1024, 2048], P('fs', 'tp')
The draws below stay inside these ranges and needn't reach their ends.
Inputs may be any that keep to these rules, and one draw needn't show every extreme that they name: `route_ids`: each row names 2 different experts of one group, numbers g * 4 to g * 4 + 3 for some g. In each aligned block of 128 rows (the rows of one index of fs) no expert is named by more than 32 rows, and some experts are named by exactly 32 rows in every block.
All inputs are finite; a program needn't handle non-finite values.
Results may differ from the reference program's by a relative error of at most 0.015.
Values may be sent and summed in bfloat16 or wider, within the bound.
A program may use at most 64 MiB of HBM per device.

```python
import jax
import jax.numpy as jnp
from jax import lax

D = 2048
H = 1024
GROUPS = 4
TOP = 2
TOK_DEV = 128
EXPERTS = 16
CAP = 32
TOKENS = 1024
N_TP = 4


def shuffle_table(table_key):
    return jax.random.permutation(table_key, EXPERTS // GROUPS)


def draw_route_ids(key, part):
    per_group = EXPERTS // GROUPS
    heavy_group = jax.random.randint(jax.random.fold_in(key, 11), (), 0, GROUPS)

    def one_block(block_number):
        block_key = jax.random.fold_in(jax.random.fold_in(key, 23), block_number)
        shuffled = jax.random.permutation(jax.random.fold_in(block_key, 1), TOK_DEV)
        other_shift = jax.random.randint(jax.random.fold_in(block_key, 2), (TOK_DEV,), 1, GROUPS)
        ranked = jnp.zeros((TOK_DEV,), jnp.int32).at[shuffled].set(jnp.arange(TOK_DEV, dtype=jnp.int32))
        group_ids = jnp.where(ranked < TOK_DEV // 2, heavy_group, (heavy_group + other_shift) % GROUPS)
        onehot = (group_ids[:, None] == jnp.arange(GROUPS, dtype=jnp.int32)[None, :]).astype(jnp.int32)
        rank_in = jnp.sum((jnp.cumsum(onehot, axis=0) - onehot) * onehot, axis=1)
        offsets = jax.random.randint(jax.random.fold_in(block_key, 3), (GROUPS,), 0, per_group)
        tables = jax.vmap(shuffle_table)(jax.random.split(jax.random.fold_in(block_key, 4), GROUPS))
        position = 2 * rank_in + jnp.sum(onehot * offsets[None, :], axis=1)
        first_slot = position % per_group
        second_slot = (position + 1) % per_group
        row_table = tables[group_ids]
        pick_first = jnp.take_along_axis(row_table, first_slot[:, None], axis=1)
        pick_second = jnp.take_along_axis(row_table, second_slot[:, None], axis=1)
        return jnp.concatenate([pick_first, pick_second], axis=1) + group_ids[:, None] * per_group
    blocks = jax.vmap(one_block)(jnp.arange(TOKENS // TOK_DEV, dtype=jnp.int32))
    return blocks.reshape(TOKENS, TOP).astype(jnp.int32)


def block_levels(stream_key, dims, cuts, least, largest):
    factor_of = 1.0
    for dim, blocks in cuts:
        draws = jax.random.uniform(jax.random.fold_in(jax.random.fold_in(stream_key, 6), dim), (blocks,), jnp.float32, least / len(cuts), largest / len(cuts))
        factor_of = factor_of * jnp.repeat(jnp.exp(draws), dims[dim] // blocks).reshape((-1,) + (1,) * (len(dims) - 1 - dim))
    return factor_of


def bell_draw(stream_key, shape, deviation, reach, cuts=(), kind=jnp.bfloat16):
    array = jax.random.normal(stream_key, shape, jnp.float32) * deviation
    if len(cuts) > 0:
        array = block_levels(stream_key, shape, cuts, -0.22, 0.18) * array
    return jnp.clip(array, min=-reach, max=reach).astype(kind)


def setup_inputs(seed: int = 0) -> dict:
    key_list = jax.random.split(jax.random.key(seed), 8)
    return {
        "tokens": bell_draw(key_list[0], (TOKENS, D), 1.0, 6.0, ((0, 8),)),
        "route_ids": draw_route_ids(jax.random.fold_in(key_list[7], 71), 0),
        "route_weights": jnp.clip(0.05 + 0.55 * jax.random.uniform(key_list[2], (TOKENS, TOP), jnp.float32) ** block_levels(key_list[2], (TOKENS, TOP), ((0, 8),), -0.2, 0.2), 0.05, 0.6),
        "norm_gain": jnp.clip(1.0 + 0.18 * jax.random.normal(key_list[3], (D,), jnp.float32), 0.1, 1.9),
        "gate_weight": bell_draw(key_list[4], (EXPERTS, D, H), 1.0, 6.0, ((1, 8), (2, 4)), jnp.float32),
        "up_weight": bell_draw(key_list[5], (EXPERTS, D, H), 1.0, 6.0, ((1, 8), (2, 4)), jnp.float32),
        "down_weight": bell_draw(key_list[6], (EXPERTS, D, H), 1.0, 6.0, ((1, 8), (2, 4)), jnp.float32),
    }


epsilon = 1e-06

def slot_positions(route_ids):
    blocked = route_ids.reshape(TOKENS // TOK_DEV, TOK_DEV * TOP)
    onehot = (blocked[:, :, None] == jnp.arange(EXPERTS, dtype=jnp.int32)[None, None, :]).astype(jnp.int32)
    earlier = jnp.cumsum(onehot, axis=1) - onehot
    return lax.optimization_barrier(jnp.sum(earlier * onehot, axis=2)).reshape(TOKENS, TOP).astype(jnp.int32)

def reference(tokens, route_ids, route_weights, norm_gain, gate_weight, up_weight, down_weight):
    scaling = norm_gain[:, None]
    gate_served = (scaling * gate_weight).astype(jnp.bfloat16)
    up_served = (scaling * up_weight).astype(jnp.bfloat16)
    down_served = down_weight.astype(jnp.bfloat16)
    widened = tokens.astype(jnp.float32)
    normed = (widened * lax.rsqrt(lax.optimization_barrier(jnp.mean(widened * widened, axis=1, keepdims=True)) + epsilon)).astype(jnp.bfloat16)
    block_index = (jnp.arange(TOKENS, dtype=jnp.int32) // TOK_DEV)[:, None]
    slot_index = (block_index * CAP + slot_positions(route_ids)).astype(jnp.int32)
    slot_rows = TOKENS // TOK_DEV * CAP
    token_of = jnp.broadcast_to(jnp.arange(TOKENS, dtype=jnp.int32)[:, None], (TOKENS, TOP))
    row_owner = jnp.zeros((EXPERTS, slot_rows), jnp.int32).at[route_ids, slot_index].set(token_of)

    def expert(operands):
        gate_one, up_one, down_one, owners = operands
        inputs = normed[owners]
        gate_pre = jnp.dot(inputs, gate_one, preferred_element_type=jnp.float32) * D ** (-0.5)
        up_pre = jnp.dot(inputs, up_one, preferred_element_type=jnp.float32) * D ** (-0.5)
        hidden = (jax.nn.silu(gate_pre) * up_pre).astype(jnp.bfloat16)
        blocks_h = hidden.astype(jnp.float32).reshape(slot_rows, N_TP, H // N_TP)
        blocks_d = down_one.astype(jnp.float32).reshape(D, N_TP, H // N_TP)
        partial_value = (jnp.einsum('rtj,dtj->trd', blocks_h, blocks_d) * H ** (-0.5)).astype(jnp.bfloat16)
        return lax.optimization_barrier(jnp.sum(partial_value.astype(jnp.float32), axis=0)).astype(jnp.bfloat16)
    expert_outs = lax.map(expert, (gate_served, up_served, down_served, row_owner))
    picked = expert_outs[route_ids, slot_index].astype(jnp.float32)
    combined = lax.optimization_barrier(jnp.sum(route_weights[:, :, None] * picked, axis=1))
    return (gate_served, up_served, down_served, combined.astype(jnp.bfloat16))
```

```python
import functools

import jax
import jax.numpy as jnp
from jax import lax
from jax.experimental import pallas as pl
from jax.experimental.pallas import tpu as pltpu
from jax.sharding import PartitionSpec as P

GROUPS = 4
EPSILON = 1e-06
MESH = pl.DeviceIdType.MESH
F32, BF16, I32 = jnp.float32, jnp.bfloat16, jnp.int32


def matmul(a, b, contract=((1,), (0,))):
    return lax.dot_general(a, b, (contract, ((), ())), preferred_element_type=F32)


def kernel(
    nf, nt,
    tokens, ids, ids_t, weights, gain, gate, up, down,
    gate_out, up_out, down_out, combined,
    wf, ws, wr, xs, xr, hs, ps, pr, rs, ret,
    load_sem, wsend, wrecv, xsend, xrecv, gsend, grecv, psend, precv, rsend, rrecv, out_sem,
):
    f, t = lax.axis_index("fs"), lax.axis_index("tp")
    experts, rows, hidden = gate.shape
    n_tok, d_model = tokens.shape
    per = experts // nf
    cap = n_tok * GROUPS // experts
    cols = d_model // nt
    slots = experts * cap
    per_owner = cols // rows
    step = jnp.where(f < nf // 2, 1, nf - 1)

    def peer(k):
        return lax.rem(f + k * step, nf)

    def other(k):
        return lax.rem(t + k, nt)

    def loads(a, k):
        p = peer(k)
        block = pl.ds(p * per, per)
        return pltpu.make_async_copy(
            (gate, up, down)[a].at[block], wf.at[a, block], load_sem.at[a, k]
        )

    def weight_copy(a, p, source):
        return pltpu.make_async_remote_copy(
            src_ref=ws.at[a, pl.ds(p * per, per)],
            dst_ref=wr.at[a, :, pl.ds(pl.multiple_of(source * rows, rows), rows), :],
            send_sem=wsend.at[a, p],
            recv_sem=wrecv.at[a, source],
            device_id={"fs": p},
            device_id_type=MESH,
        )

    def token_copy(p, source):
        return pltpu.make_async_remote_copy(
            src_ref=xs.at[pl.ds(p * per, per)],
            dst_ref=xr.at[t, :, pl.ds(pl.multiple_of(source * cap, cap), cap), :],
            send_sem=xsend.at[p],
            recv_sem=xrecv.at[source],
            device_id={"fs": p},
            device_id_type=MESH,
        )

    def gather_copy(o, source):
        return pltpu.make_async_remote_copy(
            src_ref=xr.at[source],
            dst_ref=xr.at[source],
            send_sem=gsend.at[o],
            recv_sem=grecv.at[source],
            device_id={"tp": o},
            device_id_type=MESH,
        )

    def partial_copy(o, source):
        return pltpu.make_async_remote_copy(
            src_ref=ps.at[o],
            dst_ref=pr.at[source],
            send_sem=psend.at[o],
            recv_sem=precv.at[source],
            device_id={"tp": o},
            device_id_type=MESH,
        )

    def return_copy(p, source):
        return pltpu.make_async_remote_copy(
            src_ref=rs.at[:, pl.ds(pl.multiple_of(p * cap, cap), cap), :],
            dst_ref=ret.at[pl.ds(source * per, per)],
            send_sem=rsend.at[p],
            recv_sem=rrecv.at[source],
            device_id={"fs": p},
            device_id_type=MESH,
        )

    def each(first, last, action):
        def go(k, carry):
            action(k)
            return carry
        lax.fori_loop(first, last, go, 0)

    for a in range(3):
        each(1, nf, lambda k: loads(a, k).start())
        loads(a, 0).start()

    barrier = pltpu.get_barrier_semaphore()
    each(1, nf, lambda k: pl.semaphore_signal(
        barrier, inc=1, device_id={"fs": peer(k)}, device_id_type=MESH))
    each(1, nt, lambda k: pl.semaphore_signal(
        barrier, inc=1, device_id={"tp": other(k)}, device_id_type=MESH))
    pl.semaphore_wait(barrier, nf + nt - 2)

    def converted(a, p):
        value = wf[a, pl.ds(p * per, per)]
        if a < 2:
            value = value * gain[...][None]
        return value.astype(BF16)

    def send_weights(a):
        def one(k):
            p = peer(k)
            loads(a, k).wait()
            ws[a, pl.ds(p * per, per)] = converted(a, p)
            weight_copy(a, p, f).start()
        each(1, nf, one)
        loads(a, 0).wait()
        wr[a, :, pl.ds(pl.multiple_of(f * rows, rows), rows), :] = converted(a, f)

    send_weights(0)

    wide = tokens[...].astype(F32)
    scale = lax.rsqrt(jnp.mean(wide * wide, axis=1, keepdims=True) + EPSILON)
    own = tokens[:, pl.ds(pl.multiple_of(t * cols, cols), cols)].astype(F32)
    normed = (own * scale).astype(BF16)
    slot = lax.broadcasted_iota(I32, (slots, n_tok), 0)
    slot_expert, slot_place = slot // cap, slot % cap
    named = (ids_t[0:1, :] == slot_expert) | (ids_t[1:2, :] == slot_expert)
    earlier = (
        lax.broadcasted_iota(I32, (n_tok, n_tok), 0) < lax.broadcasted_iota(I32, (n_tok, n_tok), 1)
    )
    place = matmul(named.astype(F32).astype(BF16), earlier.astype(F32).astype(BF16))
    chosen = named & (place.astype(I32) == slot_place)
    picked = matmul(chosen.astype(F32).astype(BF16), normed)
    xs[...] = picked.reshape(experts, cap, cols).astype(BF16)
    each(1, nf, lambda k: token_copy(peer(k), f).start())
    own_rows = pl.ds(pl.multiple_of(f * cap, cap), cap)
    xr[t, :, own_rows, :] = xs[pl.ds(f * per, per)]

    send_weights(1)
    send_weights(2)

    each(1, nf, lambda k: token_copy(f, peer(k)).wait_recv())
    each(1, nt, lambda k: gather_copy(other(k), t).start())
    each(1, nt, lambda k: gather_copy(t, other(k)).wait_recv())

    def product(a, e):
        total = jnp.zeros((nf * cap, hidden), F32)
        for o in range(nt):
            total += matmul(xr[o, e], wr[a, e, o * cols:(o + 1) * cols, :])
        return total * d_model ** (-0.5)

    outs = [pltpu.make_async_copy(wr.at[a], (gate_out, up_out, down_out)[a], out_sem.at[a])
            for a in range(3)]
    each(1, nf, lambda k: weight_copy(0, f, peer(k)).wait_recv())
    outs[0].start()
    gates = [product(0, e) for e in range(per)]
    each(1, nf, lambda k: weight_copy(1, f, peer(k)).wait_recv())
    outs[1].start()
    for e in range(per):
        ups = product(1, e)
        v = gates[e]
        hs[e] = (v / (1.0 + jnp.exp(-v)) * ups).astype(BF16)

    hidden_scale = (hidden * nt) ** (-0.5)

    def block(j):
        o = jnp.where(f < nf // 2, j, nt - 1 - j)

        def arrived(i):
            s = o * per_owner + i

            @pl.when(s != f)
            def _():
                weight_copy(2, f, s).wait_recv()
        each(0, per_owner, arrived)
        for e in range(per):
            tile = wr[2, e, pl.ds(pl.multiple_of(o * cols, cols), cols), :]
            part = matmul(hs[e], tile, ((1,), (1,))) * hidden_scale
            ps[o, e] = part.astype(BF16)

        @pl.when(o != t)
        def _():
            partial_copy(o, t).start()
    each(0, nt, block)
    outs[2].start()

    for e in range(per):
        pr[t, e] = ps[t, e]
    each(1, nt, lambda k: partial_copy(t, other(k)).wait_recv())
    for e in range(per):
        total = pr[0, e].astype(F32)
        for o in range(1, nt):
            total += pr[o, e].astype(F32)
        rs[e] = total.astype(BF16)
    each(1, nf, lambda k: return_copy(peer(k), f).start())
    ret[pl.ds(f * per, per)] = rs[:, own_rows, :]

    slot = lax.broadcasted_iota(I32, (n_tok, slots), 1)
    slot_expert, slot_place = slot // cap, slot % cap
    first, second = ids[:, 0:1] == slot_expert, ids[:, 1:2] == slot_expert
    earlier = (
        lax.broadcasted_iota(I32, (n_tok, n_tok), 1) < lax.broadcasted_iota(I32, (n_tok, n_tok), 0)
    )
    place = matmul(earlier.astype(F32).astype(BF16), (first | second).astype(F32).astype(BF16))
    share = jnp.where(first, weights[:, 0:1], jnp.where(second, weights[:, 1:2], 0.0))
    share = jnp.where(place.astype(I32) == slot_place, share, 0.0)
    high = share.astype(BF16)
    low = (share - high.astype(F32)).astype(BF16)
    each(1, nf, lambda k: return_copy(f, peer(k)).wait_recv())
    back = ret[...].astype(F32).reshape(slots, cols).astype(BF16)
    combined[...] = (matmul(high, back) + matmul(low, back)).astype(BF16)

    def drain(k):
        p = peer(k)
        for a in range(3):
            weight_copy(a, p, f).wait_send()
        token_copy(p, f).wait_send()
        return_copy(p, f).wait_send()
    each(1, nf, drain)

    def drain_tp(k):
        gather_copy(other(k), t).wait_send()
        partial_copy(other(k), t).wait_send()
    each(1, nt, drain_tp)
    for copy in outs:
        copy.wait()


def body(nf, nt, tokens, route_ids, route_weights, norm_gain, gate_weight, up_weight, down_weight):
    experts, rows, hidden = gate_weight.shape
    n_tok, d_model = tokens.shape
    per = experts // nf
    cap = n_tok * GROUPS // experts
    cols = d_model // nt
    served = jax.ShapeDtypeStruct((per, nf * rows, hidden), BF16)
    vmem, anywhere = pl.BlockSpec(memory_space=pltpu.VMEM), pl.BlockSpec(memory_space=pl.ANY)
    dma = pltpu.SemaphoreType.DMA
    return pl.pallas_call(
        functools.partial(kernel, nf, nt),
        out_shape=(served, served, served, jax.ShapeDtypeStruct((n_tok, cols), BF16)),
        in_specs=[vmem] * 5 + [anywhere] * 3,
        out_specs=(anywhere, anywhere, anywhere, vmem),
        scratch_shapes=[
            pltpu.VMEM((3, experts, rows, hidden), F32),
            pltpu.VMEM((3, experts, rows, hidden), BF16),
            pltpu.VMEM((3, per, nf * rows, hidden), BF16),
            pltpu.VMEM((experts, cap, cols), BF16),
            pltpu.VMEM((nt, per, nf * cap, cols), BF16),
            pltpu.VMEM((per, nf * cap, hidden), BF16),
            pltpu.VMEM((nt, per, nf * cap, cols), BF16),
            pltpu.VMEM((nt, per, nf * cap, cols), BF16),
            pltpu.VMEM((per, nf * cap, cols), BF16),
            pltpu.VMEM((experts, cap, cols), BF16),
            dma((3, nf)),
            dma((3, nf)), dma((3, nf)),
            dma((nf,)), dma((nf,)),
            dma((nt,)), dma((nt,)),
            dma((nt,)), dma((nt,)),
            dma((nf,)), dma((nf,)),
            dma((3,)),
        ],
        compiler_params=pltpu.CompilerParams(
            collective_id=0, has_side_effects=True, vmem_limit_bytes=56 * 1024 * 1024
        ),
    )(
        tokens, route_ids, route_ids.T, route_weights, norm_gain[:, None],
        gate_weight, up_weight, down_weight,
    )


def solution(mesh):
    split = P(None, "fs", "tp")
    served = P("fs", None, "tp")
    return jax.shard_map(
        functools.partial(body, mesh.shape["fs"], mesh.shape["tp"]),
        mesh=mesh,
        in_specs=(P("fs", None), P("fs", None), P("fs", None), P("fs"), split, split, split),
        out_specs=(served, served, served, P("fs", "tp")),
        check_vma=False,
    )
```

```python
import functools

import jax
import jax.numpy as jnp
from jax import lax
from jax.experimental import pallas as pl
from jax.experimental.pallas import tpu as pltpu
from jax.sharding import PartitionSpec as P

GROUPS = 4
EPSILON = 1e-06
MESH = pl.DeviceIdType.MESH
LAG = 2
F32, BF16, I32 = jnp.float32, jnp.bfloat16, jnp.int32


def matmul(a, b, contract=((1,), (0,))):
    return lax.dot_general(a, b, (contract, ((), ())), preferred_element_type=F32)


def assignment(ids_t, experts, cap):
    n_tok = ids_t.shape[1]
    slot = lax.broadcasted_iota(I32, (experts * cap, n_tok), 0)
    first, second = ids_t[0:1, :] == slot // cap, ids_t[1:2, :] == slot // cap
    earlier = (
        lax.broadcasted_iota(I32, (n_tok, n_tok), 0) < lax.broadcasted_iota(I32, (n_tok, n_tok), 1)
    )
    named = (first | second).astype(F32).astype(BF16)
    place = matmul(named, earlier.astype(F32).astype(BF16))
    return (first | second) & (place.astype(I32) == slot % cap), first


def kernel(
    nf, nt,
    tokens, ids_t, gain, gate, up, down,
    gate_out, up_out, down_out, ret,
    wf, ws, xs, xr, hs, ps, pr, rs,
    load_sem, wsend, wrecv, xsend, xrecv, gsend, grecv, psend, precv, rsend, rrecv,
):
    f, t = lax.axis_index("fs"), lax.axis_index("tp")
    experts, rows, hidden = gate.shape
    n_tok, d_model = tokens.shape
    per = experts // nf
    cap = n_tok * GROUPS // experts
    cols = d_model // nt
    slots = experts * cap
    per_owner = cols // rows
    served = (gate_out, up_out, down_out)
    low_half = f < nf // 2

    def peer(k):
        down_to = jnp.where(k < nf - f, nf - k, nf - 1 - k)
        up_to = jnp.where(k <= f, k - 1, k)
        return jnp.where(k == 0, f, jnp.where(low_half, down_to, up_to))

    def other(k):
        return lax.rem(t + k, nt)

    def loads(e, a, k):
        n = peer(k) * per + e
        return pltpu.make_async_copy(
            (gate, up, down)[a].at[n], wf.at[a, n], load_sem.at[e, a, k]
        )

    def weight_copy(e, a, p, source):
        return pltpu.make_async_remote_copy(
            src_ref=ws.at[a, p * per + e],
            dst_ref=served[a].at[e, pl.ds(pl.multiple_of(source * rows, rows), rows), :],
            send_sem=wsend.at[e, a, p],
            recv_sem=wrecv.at[e, a, source],
            device_id={"fs": p},
            device_id_type=MESH,
        )

    def token_copy(p, source):
        return pltpu.make_async_remote_copy(
            src_ref=xs.at[pl.ds(p * per, per)],
            dst_ref=xr.at[t, :, pl.ds(pl.multiple_of(source * cap, cap), cap), :],
            send_sem=xsend.at[p],
            recv_sem=xrecv.at[source],
            device_id={"fs": p},
            device_id_type=MESH,
        )

    def gather_copy(o, source):
        return pltpu.make_async_remote_copy(
            src_ref=xr.at[source],
            dst_ref=xr.at[source],
            send_sem=gsend.at[o],
            recv_sem=grecv.at[source],
            device_id={"tp": o},
            device_id_type=MESH,
        )

    def partial_copy(e, s, source):
        return pltpu.make_async_remote_copy(
            src_ref=ps.at[e, s],
            dst_ref=pr.at[source, e, lax.rem(s, per_owner)],
            send_sem=psend.at[e, s],
            recv_sem=precv.at[source, e, lax.rem(s, per_owner)],
            device_id={"tp": s // per_owner},
            device_id_type=MESH,
        )

    def return_copy(e, p, source, i):
        return pltpu.make_async_remote_copy(
            src_ref=rs.at[e, i, pl.ds(pl.multiple_of(p * cap, cap), cap), :],
            dst_ref=ret.at[i, source * per + e],
            send_sem=rsend.at[e, i, p],
            recv_sem=rrecv.at[e, i, source],
            device_id={"fs": p},
            device_id_type=MESH,
        )

    def each(first, last, action):
        def go(k, carry):
            action(k)
            return carry
        lax.fori_loop(first, last, go, 0)

    each(1, nf, lambda k: loads(0, 0, k).start())
    loads(0, 0, 0).start()

    barrier = pltpu.get_barrier_semaphore()
    each(1, nf, lambda k: pl.semaphore_signal(
        barrier, inc=1, device_id={"fs": peer(k)}, device_id_type=MESH))
    each(1, nt, lambda k: pl.semaphore_signal(
        barrier, inc=1, device_id={"tp": other(k)}, device_id_type=MESH))
    pl.semaphore_wait(barrier, nf + nt - 2)

    square = lax.broadcasted_iota(I32, (rows, rows), 0) == lax.broadcasted_iota(I32, (rows, rows), 1)
    gain_column = jnp.sum(jnp.where(square, gain[...], 0.0), axis=1, keepdims=True)

    def converted(a, n):
        value = wf[a, n]
        if a < 2:
            value = value * gain_column
        return value.astype(BF16)

    def send_weights(e, a):
        e_next, a_next = (e, a + 1) if a < 2 else (e + 1, 0)

        def load_next(k):
            if e_next < per:
                loads(e_next, a_next, k).start()

        def one(k):
            p = peer(k)
            loads(e, a, k).wait()
            load_next(k)
            ws[a, p * per + e] = converted(a, p * per + e)
            weight_copy(e, a, p, f).start()
        each(1, nf, one)
        loads(e, a, 0).wait()
        load_next(0)
        served[a][e, pl.ds(pl.multiple_of(f * rows, rows), rows), :] = converted(a, f * per + e)

    send_weights(0, 0)

    wide = tokens[...].astype(F32)
    scale = lax.rsqrt(jnp.mean(wide * wide, axis=1, keepdims=True) + EPSILON)
    own = tokens[:, pl.ds(pl.multiple_of(t * cols, cols), cols)].astype(F32)
    normed = (own * scale).astype(BF16)
    chosen, _ = assignment(ids_t, experts, cap)
    picked = matmul(chosen.astype(F32).astype(BF16), normed)
    xs[...] = picked.reshape(experts, cap, cols).astype(BF16)
    each(1, nf, lambda k: token_copy(peer(k), f).start())
    own_rows = pl.ds(pl.multiple_of(f * cap, cap), cap)
    xr[t, :, own_rows, :] = xs[pl.ds(f * per, per)]

    for e in range(per):
        for a in range(3):
            if e + a > 0:
                send_weights(e, a)

    each(1, nf, lambda k: token_copy(f, peer(k)).wait_recv())
    each(1, nt, lambda k: gather_copy(other(k), t).start())
    each(1, nt, lambda k: gather_copy(t, other(k)).wait_recv())

    def product(a, e):
        total = jnp.zeros((nf * cap, hidden), F32)
        for o in range(nt):
            total += matmul(xr[o, e], served[a][e, o * cols:(o + 1) * cols, :])
        return total * d_model ** (-0.5)

    hidden_scale = (hidden * nt) ** (-0.5)

    def block_at(j):
        return jnp.where(low_half, j, nf - 1 - j)

    def block(e, j):
        s = block_at(j)

        @pl.when(s != f)
        def _():
            weight_copy(e, 2, f, s).wait_recv()
        tile = down_out[e, pl.ds(pl.multiple_of(s * rows, rows), rows), :]
        ps[e, s] = (matmul(hs[...], tile, ((1,), (1,))) * hidden_scale).astype(BF16)

        @pl.when(s // per_owner != t)
        def _():
            partial_copy(e, s, t).start()

    def finish(e, j):
        s = block_at(j)
        i = lax.rem(s, per_owner)

        @pl.when(s // per_owner == t)
        def _():
            each(1, nt, lambda k: partial_copy(e, s, other(k)).wait_recv())
            total = ps[e, s].astype(F32)
            for k in range(1, nt):
                total += pr[other(k), e, i].astype(F32)
            rs[e, i] = total.astype(BF16)
            each(1, nf, lambda k: return_copy(e, peer(k), f, i).start())
            ret[i, f * per + e] = rs[e, i, own_rows, :]

    for e in range(per):
        each(1, nf, lambda k: weight_copy(e, 0, f, peer(k)).wait_recv())
        v = product(0, e)
        each(1, nf, lambda k: weight_copy(e, 1, f, peer(k)).wait_recv())
        hs[...] = (v / (1.0 + jnp.exp(-v)) * product(1, e)).astype(BF16)

        each(0, LAG, lambda j: block(e, j))

        def both(j):
            block(e, j)
            finish(e, j - LAG)
        each(LAG, nf, both)
        each(nf - LAG, nf, lambda j: finish(e, j))
    for e in range(per):
        each(0, per_owner, lambda i: each(
            1, nf, lambda k: return_copy(e, f, peer(k), i).wait_recv()))

    def drain(k):
        p = peer(k)
        for e in range(per):
            for a in range(3):
                weight_copy(e, a, p, f).wait_send()
            each(0, per_owner, lambda i: return_copy(e, p, f, i).wait_send())
        token_copy(p, f).wait_send()
    each(1, nf, drain)
    each(1, nt, lambda k: gather_copy(other(k), t).wait_send())

    def drain_partial(s):
        @pl.when(s // per_owner != t)
        def _():
            for e in range(per):
                partial_copy(e, s, t).wait_send()
    each(0, nf, drain_partial)


def finish_kernel(
    ids_t, weights_t, ret, gate, up, down, gate_out, up_out, down_out, combined, sem
):
    outs = [
        pltpu.make_async_copy(source, target, sem.at[a])
        for a, (source, target) in enumerate(((gate, gate_out), (up, up_out), (down, down_out)))
    ]
    for copy in outs:
        copy.start()
    chunks, experts, cap, width = ret.shape
    chosen, first = assignment(ids_t, experts, cap)
    share = jnp.where(chosen, jnp.where(first, weights_t[0:1, :], weights_t[1:2, :]), 0.0).T
    high = share.astype(BF16)
    low = (share - high.astype(F32)).astype(BF16)
    for i in range(chunks):
        back = ret[i].astype(F32).reshape(experts * cap, width).astype(BF16)
        value = matmul(high, back) + matmul(low, back)
        combined[:, i * width:(i + 1) * width] = value.astype(BF16)
    for copy in outs:
        copy.wait()


def body(nf, nt, tokens, route_ids, route_weights, norm_gain, gate_weight, up_weight, down_weight):
    experts, rows, hidden = gate_weight.shape
    n_tok, d_model = tokens.shape
    per = experts // nf
    cap = n_tok * GROUPS // experts
    cols = d_model // nt
    shape = (per, nf * rows, hidden)
    vmem, anywhere = pl.BlockSpec(memory_space=pltpu.VMEM), pl.BlockSpec(memory_space=pl.ANY)
    dma = pltpu.SemaphoreType.DMA
    per_owner = cols // rows
    ids_t, weights_t = route_ids.T, route_weights.T
    *served, ret = pl.pallas_call(
        functools.partial(kernel, nf, nt),
        out_shape=[pltpu.VMEM(shape, BF16)] * 3 + [pltpu.VMEM((per_owner, experts, cap, rows), BF16)],
        in_specs=[vmem] * 3 + [anywhere] * 3,
        out_specs=[vmem] * 4,
        scratch_shapes=[
            pltpu.VMEM((3, experts, rows, hidden), F32),
            pltpu.VMEM((3, experts, rows, hidden), BF16),
            pltpu.VMEM((experts, cap, cols), BF16),
            pltpu.VMEM((nt, per, nf * cap, cols), BF16),
            pltpu.VMEM((nf * cap, hidden), BF16),
            pltpu.VMEM((per, nf, nf * cap, rows), BF16),
            pltpu.VMEM((nt, per, per_owner, nf * cap, rows), BF16),
            pltpu.VMEM((per, per_owner, nf * cap, rows), BF16),
            dma((per, 3, nf)),
            dma((per, 3, nf)), dma((per, 3, nf)),
            dma((nf,)), dma((nf,)),
            dma((nt,)), dma((nt,)),
            dma((per, nf)), dma((nt, per, per_owner)),
            dma((per, per_owner, nf)), dma((per, per_owner, nf)),
        ],
        compiler_params=pltpu.CompilerParams(
            collective_id=0, has_side_effects=True, vmem_limit_bytes=54 * 1024 * 1024
        ),
    )(tokens, ids_t, norm_gain[None, :], gate_weight, up_weight, down_weight)
    out = jax.ShapeDtypeStruct(shape, BF16)
    return pl.pallas_call(
        finish_kernel,
        out_shape=(out, out, out, jax.ShapeDtypeStruct((n_tok, cols), BF16)),
        in_specs=[vmem] * 6,
        out_specs=(anywhere, anywhere, anywhere, vmem),
        scratch_shapes=[dma((3,))],
        compiler_params=pltpu.CompilerParams(vmem_limit_bytes=16 * 1024 * 1024),
    )(ids_t, weights_t, ret, *served)


def solution(mesh):
    split = P(None, "fs", "tp")
    served = P("fs", None, "tp")
    return jax.shard_map(
        functools.partial(body, mesh.shape["fs"], mesh.shape["tp"]),
        mesh=mesh,
        in_specs=(P("fs", None), P("fs", None), P("fs", None), P("fs"), split, split, split),
        out_specs=(served, served, served, P("fs", "tp")),
        check_vma=False,
    )
```
